32 devices in a mesh: dp: 4 (over y, x), kv: 4 (over z), tp: 2 (over core).
Axes of the slice: x: 2, y: 2, z: 4, core: 2. Of those that a mesh axis runs over, the one named last changes fastest.
Arguments:
- tokens: bfloat16 [4, 1280, 2048], P('dp', 'kv'), may hold values from -72 to 72
- w_query: bfloat16 [2048, 512], P(None, 'tp'), may hold values from -0.125 to 0.125
- key_weight: bfloat16 [2048, 256], P(None, 'tp'), may hold values from -0.125 to 0.125
- value_weight: bfloat16 [2048, 256], P(None, 'tp'), may hold values from -2.09375 to 2.09375
- w_out: bfloat16 [512, 2048], P(None, 'tp'), may hold values from -0.25 to 0.25
- chosen: int32 [4, 40, 16], P('dp', 'kv'), may hold values from -1 to 39, as said below
Outputs:
- mixed: bfloat16 [4, 1280, 2048], P('dp', 'kv', 'tp')
- log_mass: float32 [4, 4, 1280], P('dp', 'tp', 'kv')
The draws below stay inside these ranges and needn't reach their ends.
Inputs may be any that keep to these rules, and one draw needn't show every extreme that they name: `chosen`: entry 0 of row i of a sequence is i; the other entries are distinct blocks before i, or -1 for an empty slot. The 10 rows of one index of kv together name at most one block held by any other index of kv; this bound is reached.
All inputs are finite; a program needn't handle non-finite values.
Results may differ from the reference program's by a relative error of at most 0.006.
The reference program's roundings to bfloat16 on the way (of `queries`, `probs_low` and `attended`) count: a program that leaves them out, or rounds other values in their place, can miss the bound.
Values may be sent and summed in bfloat16 or wider, within the bound.
No kernel may reach another device: no remote copies, remote signals or barrier semaphores. Data moves between devices by JAX's collectives and lax.ppermute only.
A program may use at most 64 MiB of HBM per device.

```python
import jax
import jax.numpy as jnp
from jax import lax

MODEL_WIDTH = 2048
HEAD_WIDTH = 128
QUERY_HEAD_COUNT = 4
KEY_VALUE_HEADS = 2
BLOCK_POSITIONS = 32
CHOSEN_SLOTS = 16
BLK_DEV = 10
SEQUENCE_BLOCKS = 40
SEQ = 1280
SEQS = 4
N_KV = 4


def draw_tokens(key, part):
    base = jnp.clip(jax.random.normal(jax.random.fold_in(key, 21), (SEQS, SEQ, MODEL_WIDTH), jnp.float32), -6.0, 6.0)
    return base.astype(jnp.bfloat16)


def draw_chosen(key, part):
    popular = (jax.random.randint(jax.random.fold_in(key, 11), (SEQS, 1, N_KV), 0, 6) == 0).astype(jnp.int32)
    noise = jax.random.randint(jax.random.fold_in(key, 12), (SEQS, N_KV, N_KV), 0, 65536)
    block_pick = jax.random.randint(jax.random.fold_in(key, 13), (SEQS, N_KV, N_KV), 0, BLK_DEV)
    device_ix = jnp.arange(N_KV, dtype=jnp.int32)[:, None]
    owner_ix = jnp.arange(N_KV, dtype=jnp.int32)[None, :]
    forced = ((owner_ix == device_ix - 1) | (owner_ix == device_ix - N_KV // 2)).astype(jnp.int32)
    ranks = (forced * 3 + popular) * 65536 + noise
    ranks = jnp.where(owner_ix < device_ix, ranks, -1)
    ranking = jnp.argsort(-ranks, axis=-1, stable=True).astype(jnp.int32)
    spare = CHOSEN_SLOTS - BLK_DEV
    rows_out = []
    for inner_ix in range(BLK_DEV):
        slot_ix = inner_ix * spare + jnp.arange(spare, dtype=jnp.int32)
        live_slot = slot_ix[None, :] < device_ix
        bounded_index = jnp.minimum(slot_ix, N_KV - 1)
        chosen_owner = jnp.take(ranking, bounded_index, axis=2)
        chosen_block = chosen_owner * BLK_DEV + jnp.take_along_axis(block_pick, chosen_owner, axis=2)
        far_part = jnp.where(live_slot[None], chosen_block, -1)
        own_block = jnp.broadcast_to((device_ix * BLK_DEV + inner_ix)[None], (SEQS, N_KV, 1))
        near_cols = []
        for earlier in range(BLK_DEV - 1):
            column = jnp.where(earlier < inner_ix, device_ix * BLK_DEV + earlier, -1)
            near_cols.append(jnp.broadcast_to(column[None], (SEQS, N_KV, 1)))
        rows_out.append(jnp.concatenate([own_block] + near_cols + [far_part], axis=2))
    return jnp.stack(rows_out, axis=2).reshape(SEQS, SEQUENCE_BLOCKS, CHOSEN_SLOTS).astype(jnp.int32)


def shard_levels(rng, extent, cuts, low, high):
    def one(axis_at, shards_of):
        steps = jax.random.uniform(jax.random.fold_in(jax.random.fold_in(rng, 6), axis_at), (shards_of,), jnp.float32, low / len(cuts), high / len(cuts))
        return jnp.repeat(jnp.exp(steps), extent[axis_at] // shards_of).reshape((-1,) + (1,) * (len(extent) - axis_at - 1))

    level = one(*cuts[0])
    for cut in cuts[1:]:
        level = level * one(*cut)
    return level


def centred(rng, extent, scale, most, pieces=(), kind=jnp.bfloat16):
    drawn = scale * jax.random.normal(rng, extent, jnp.float32)
    if pieces:
        drawn = drawn * shard_levels(rng, extent, pieces, -0.22, 0.18)
    return jnp.clip(drawn, -most, most).astype(kind)


def setup_inputs(seed: int = 0) -> dict:
    arg_keys = jax.random.split(jax.random.key(seed), 7)
    return {
        "tokens": draw_tokens(jax.random.fold_in(arg_keys[6], 71), 0),
        "w_query": centred(arg_keys[1], (MODEL_WIDTH, QUERY_HEAD_COUNT * HEAD_WIDTH), MODEL_WIDTH ** -0.5, 0.125, ((1, 2),)),
        "key_weight": centred(arg_keys[2], (MODEL_WIDTH, KEY_VALUE_HEADS * HEAD_WIDTH), MODEL_WIDTH ** -0.5, 0.125, ((1, 2),)),
        "value_weight": centred(arg_keys[3], (MODEL_WIDTH, KEY_VALUE_HEADS * HEAD_WIDTH), 0.35, 2.09375, ((1, 2),)),
        "w_out": centred(arg_keys[4], (QUERY_HEAD_COUNT * HEAD_WIDTH, MODEL_WIDTH), (QUERY_HEAD_COUNT * HEAD_WIDTH) ** -0.5, 0.25, ((1, 2),)),
        "chosen": draw_chosen(jax.random.fold_in(arg_keys[6], 71), 0),
    }


def attend_block(entry, key_block_table, value_block_table):
    query_block_rows, row_chosen, block_index = entry
    heads_per_group = QUERY_HEAD_COUNT // KEY_VALUE_HEADS
    bounded_index = jnp.maximum(row_chosen, 0)
    selected_keys = key_block_table[bounded_index].reshape(CHOSEN_SLOTS * BLOCK_POSITIONS, KEY_VALUE_HEADS, HEAD_WIDTH)
    selected_values = value_block_table[bounded_index].reshape(CHOSEN_SLOTS * BLOCK_POSITIONS, KEY_VALUE_HEADS, HEAD_WIDTH)
    grouped_queries = query_block_rows.reshape(BLOCK_POSITIONS, KEY_VALUE_HEADS, heads_per_group, HEAD_WIDTH)
    scores = jnp.einsum('tkgd,skd->kgts', grouped_queries.astype(jnp.float32), selected_keys.astype(jnp.float32)) * (HEAD_WIDTH ** -0.5)
    key_pos = (bounded_index[:, None] * BLOCK_POSITIONS + jnp.arange(BLOCK_POSITIONS, dtype=jnp.int32)[None, :]).reshape(CHOSEN_SLOTS * BLOCK_POSITIONS)
    key_live = jnp.repeat(row_chosen >= 0, BLOCK_POSITIONS)
    query_pos = block_index * BLOCK_POSITIONS + jnp.arange(BLOCK_POSITIONS, dtype=jnp.int32)
    allowed = key_live[None, :] & (key_pos[None, :] <= query_pos[:, None])
    scores = jnp.where(allowed, scores, -jnp.inf)
    row_max = jnp.max(scores, axis=-1)
    weights = jnp.exp(scores - row_max[..., None])
    row_sum = jnp.sum(weights, axis=-1)
    probs_low = lax.optimization_barrier(weights.astype(jnp.bfloat16))
    summed = jnp.einsum('kgts,skd->tkgd', probs_low.astype(jnp.float32), selected_values.astype(jnp.float32))
    attended = (summed / row_sum.transpose(2, 0, 1)[..., None]).astype(jnp.bfloat16).reshape(BLOCK_POSITIONS, QUERY_HEAD_COUNT * HEAD_WIDTH)
    log_part = (row_max + jnp.log(row_sum)).reshape(QUERY_HEAD_COUNT, BLOCK_POSITIONS)
    return attended, log_part


def reference(tokens, w_query, key_weight, value_weight, w_out, chosen):
    def one_sequence(entry):
        seq_tokens, seq_chosen = entry
        queries = jnp.dot(seq_tokens, w_query, preferred_element_type=jnp.float32).astype(jnp.bfloat16)
        projected_keys = jnp.dot(seq_tokens, key_weight, preferred_element_type=jnp.float32).astype(jnp.bfloat16)
        projected_values = jnp.dot(seq_tokens, value_weight, preferred_element_type=jnp.float32).astype(jnp.bfloat16)
        queries = queries.reshape(SEQUENCE_BLOCKS, BLOCK_POSITIONS, QUERY_HEAD_COUNT, HEAD_WIDTH)
        key_block_table = projected_keys.reshape(SEQUENCE_BLOCKS, BLOCK_POSITIONS, KEY_VALUE_HEADS, HEAD_WIDTH)
        value_block_table = projected_values.reshape(SEQUENCE_BLOCKS, BLOCK_POSITIONS, KEY_VALUE_HEADS, HEAD_WIDTH)

        def per_block(item_entry):
            return attend_block(item_entry, key_block_table, value_block_table)

        attended, log_part = lax.map(per_block, (queries, seq_chosen, jnp.arange(SEQUENCE_BLOCKS, dtype=jnp.int32)))
        attended = attended.reshape(SEQ, QUERY_HEAD_COUNT * HEAD_WIDTH)
        mixed = jnp.dot(attended, w_out, preferred_element_type=jnp.float32).astype(jnp.bfloat16)
        return mixed, log_part.transpose(1, 0, 2).reshape(QUERY_HEAD_COUNT, SEQ)

    mixed_all, log_all = lax.map(one_sequence, (tokens, chosen))
    return mixed_all, log_all
```

```python
import functools

import jax
import jax.numpy as jnp
from jax import lax
from jax.experimental import pallas as pl
from jax.experimental.pallas import tpu as pltpu
from jax.sharding import PartitionSpec as P

HEAD_WIDTH = 128
LOG2E = 1.4426950408889634
VMEM = pl.BlockSpec(memory_space=pltpu.VMEM)


def xor_distances(count):
    span = 1
    while span < count:
        span *= 2
    return list(range(1, span))


def exchange(value, distance, count):
    pairs = [(i, i ^ distance) for i in range(count) if (i ^ distance) < count]
    return lax.ppermute(value, "kv", pairs)


def pick_kernel(blocks_here, block_rows, far_count, *refs):
    kv_ref = refs[0]
    asked_refs = refs[1 : 1 + far_count]
    out_refs = refs[1 + far_count :]
    base = lax.axis_index("kv") * blocks_here
    rows = blocks_here * block_rows
    offset = lax.broadcasted_iota(jnp.int32, (block_rows, rows), 1) - lax.broadcasted_iota(
        jnp.int32, (block_rows, rows), 0
    )
    kv = kv_ref[...]
    for asked_ref, out_ref in zip(asked_refs, out_refs):
        asked = asked_ref[...]
        mine = (asked >= base) & (asked < base + blocks_here)
        local = jnp.max(jnp.where(mine, asked - base, -1), axis=(0, 1), keepdims=True)
        hot = jnp.where(offset == local * block_rows, 1.0, 0.0).astype(jnp.bfloat16)
        out_ref[...] = jnp.dot(hot, kv, preferred_element_type=jnp.float32).astype(jnp.bfloat16)


def attend_kernel(
    blocks_here, block_rows, distances, heads, chosen_ref, q_ref, kv_ref, *refs
):
    far_refs = refs[: len(distances)]
    out_ref, mass_ref = refs[len(distances) :]
    my_index = lax.axis_index("kv")
    rows = blocks_here * block_rows
    far_rows = len(distances) * block_rows
    keys = rows + far_rows
    chosen = chosen_ref[...]
    slots = chosen.shape[1]
    column = lax.broadcasted_iota(jnp.int32, (1, keys), 1)
    low = my_index * blocks_here + column // block_rows
    high = low + 1
    for at, distance in enumerate(distances):
        start = rows + at * block_rows
        here = (column >= start) & (column < start + block_rows)
        owner = jnp.bitwise_xor(my_index, distance)
        low = jnp.where(here, owner * blocks_here, low)
        high = jnp.where(here, (owner + 1) * blocks_here, high)
    member = jnp.zeros((blocks_here, keys), jnp.bool_)
    for slot in range(slots):
        entry = chosen[:, slot : slot + 1]
        member = member | ((entry >= low) & (entry < high))
    member = jnp.where(member, 1.0, 0.0).astype(jnp.bfloat16)
    spread = (
        lax.broadcasted_iota(jnp.int32, (blocks_here, rows), 1) // block_rows
        == lax.broadcasted_iota(jnp.int32, (blocks_here, rows), 0)
    )
    spread = jnp.where(spread, 1.0, 0.0).astype(jnp.bfloat16)
    named = lax.dot_general(
        member, spread, (((0,), (0,)), ((), ())), preferred_element_type=jnp.float32
    )
    key_at = lax.broadcasted_iota(jnp.int32, (keys, rows), 0)
    query_at = lax.broadcasted_iota(jnp.int32, (keys, rows), 1)
    allowed = (named > 0.5) & ((key_at <= query_at) | (key_at >= rows))
    key_rows = jnp.concatenate(
        [kv_ref[:, :HEAD_WIDTH]] + [far[:, :HEAD_WIDTH] for far in far_refs], axis=0
    )
    value_rows = jnp.concatenate(
        [kv_ref[:, HEAD_WIDTH:]] + [far[:, HEAD_WIDTH:] for far in far_refs], axis=0
    )
    scale = HEAD_WIDTH ** (-0.5)
    for head in range(heads):
        lanes = slice(head * HEAD_WIDTH, (head + 1) * HEAD_WIDTH)
        raw = lax.dot_general(
            key_rows, q_ref[:, lanes], (((1,), (1,)), ((), ())), preferred_element_type=jnp.float32
        )
        raw = jnp.where(allowed, raw, -jnp.inf)
        top = jnp.max(raw, axis=0, keepdims=True)
        weights = jnp.exp2((raw - top) * (scale * LOG2E))
        total = jnp.sum(weights, axis=0, keepdims=True)
        summed = lax.dot_general(
            value_rows,
            weights.astype(jnp.bfloat16),
            (((0,), (0,)), ((), ())),
            preferred_element_type=jnp.float32,
        )
        out_ref[:, lanes] = (summed / total).T.astype(jnp.bfloat16)
        mass_ref[head : head + 1, :] = top * scale + jnp.log(total)


def mix_kernel(own_ref, other_ref, w_ref, out_ref):
    width = own_ref.shape[1]
    side = lax.axis_index("tp")
    own_w = w_ref[pl.ds(pl.multiple_of(side * width, width), width), :]
    other_w = w_ref[pl.ds(pl.multiple_of((1 - side) * width, width), width), :]
    mixed = jnp.dot(own_ref[...], own_w, preferred_element_type=jnp.float32)
    mixed += jnp.dot(other_ref[...], other_w, preferred_element_type=jnp.float32)
    out_ref[...] = mixed.astype(jnp.bfloat16)


def body(tokens, w_query, key_weight, value_weight, w_out, chosen):
    local_tokens = tokens[0]
    local_chosen = chosen[0]
    rows = local_tokens.shape[0]
    blocks_here = local_chosen.shape[0]
    block_rows = rows // blocks_here
    heads = w_query.shape[1] // HEAD_WIDTH
    count = lax.axis_size("kv")
    distances = xor_distances(count)
    asked = [exchange(local_chosen, distance, count) for distance in distances]

    def project(weight):
        return jnp.dot(local_tokens, weight, preferred_element_type=jnp.float32).astype(
            jnp.bfloat16
        )

    paired = jnp.concatenate([project(key_weight), project(value_weight)], axis=1)
    queries = project(w_query)
    block = jax.ShapeDtypeStruct((block_rows, paired.shape[1]), jnp.bfloat16)
    picked = pl.pallas_call(
        functools.partial(pick_kernel, blocks_here, block_rows, len(distances)),
        out_shape=[block] * len(distances),
        in_specs=[VMEM] * (1 + len(distances)),
        out_specs=[VMEM] * len(distances),
        name="pick",
    )(paired, *asked)
    far = [exchange(rows_out, distance, count) for rows_out, distance in zip(picked, distances)]
    attended, log_mass = pl.pallas_call(
        functools.partial(attend_kernel, blocks_here, block_rows, distances, heads),
        out_shape=[
            jax.ShapeDtypeStruct((rows, heads * HEAD_WIDTH), jnp.bfloat16),
            jax.ShapeDtypeStruct((heads, rows), jnp.float32),
        ],
        in_specs=[VMEM] * (3 + len(distances)),
        out_specs=[VMEM] * 2,
        name="attend",
    )(local_chosen, queries, paired, *far)
    other = lax.ppermute(attended, "tp", [(0, 1), (1, 0)])
    mixed = pl.pallas_call(
        mix_kernel,
        out_shape=jax.ShapeDtypeStruct((rows, w_out.shape[1]), jnp.bfloat16),
        in_specs=[VMEM] * 3,
        out_specs=VMEM,
        name="mix",
    )(attended, other, w_out)
    return (mixed[None], log_mass[None])


def solution(mesh):
    in_specs = (
        P("dp", "kv", None),
        P(None, "tp"),
        P(None, "tp"),
        P(None, "tp"),
        P(None, "tp"),
        P("dp", "kv", None),
    )
    out_specs = (P("dp", "kv", "tp"), P("dp", "tp", "kv"))
    return jax.shard_map(body, mesh=mesh, in_specs=in_specs, out_specs=out_specs, check_vma=False)
```

```python
import functools

import jax
import jax.numpy as jnp
from jax import lax
from jax.experimental import pallas as pl
from jax.experimental.pallas import tpu as pltpu
from jax.sharding import PartitionSpec as P

HEAD_WIDTH = 128
LOG2E = 1.4426950408889634
VMEM = pl.BlockSpec(memory_space=pltpu.VMEM)


def xor_distances(count):
    span = 1
    while span < count:
        span *= 2
    return list(range(1, span))


def exchange(value, distance, count):
    pairs = [(i, i ^ distance) for i in range(count) if (i ^ distance) < count]
    return lax.ppermute(value, "kv", pairs)


def grant(*sizes):
    return pltpu.CompilerParams(vmem_limit_bytes=(4 << 20) + 4 * sum(sizes))


def pick_kernel(blocks_here, block_rows, far_count, *refs):
    kv_ref = refs[0]
    asked_refs = refs[1 : 1 + far_count]
    out_refs = refs[1 + far_count :]
    base = lax.axis_index("kv") * blocks_here
    rows = blocks_here * block_rows
    offset = lax.broadcasted_iota(jnp.int32, (block_rows, rows), 1) - lax.broadcasted_iota(
        jnp.int32, (block_rows, rows), 0
    )
    kv = kv_ref[...]
    for asked_ref, out_ref in zip(asked_refs, out_refs):
        asked = asked_ref[:, 0, :]
        mine = (asked >= base) & (asked < base + blocks_here)
        local = jnp.max(jnp.where(mine, asked - base, -1), axis=(0, 1), keepdims=True)
        hot = jnp.where(offset == local * block_rows, 1.0, 0.0).astype(jnp.bfloat16)
        out_ref[...] = jnp.dot(hot, kv, preferred_element_type=jnp.float32).astype(jnp.bfloat16)


def named_pairs(chosen, low, high, spread):
    member = (chosen[:, :1] >= low) & (chosen[:, :1] < high)
    for slot in range(1, chosen.shape[1]):
        entry = chosen[:, slot : slot + 1]
        member = member | ((entry >= low) & (entry < high))
    member = jnp.where(member, 1.0, 0.0).astype(jnp.bfloat16)
    return (
        lax.dot_general(
            member, spread, (((0,), (0,)), ((), ())), preferred_element_type=jnp.float32
        )
        > 0.5
    )


def local_kernel(
    blocks_here, block_rows, distances, heads, chosen_ref, q_ref, kv_ref,
    sum_ref, stat_ref, bias_ref,
):
    my_index = lax.axis_index("kv")
    rows = blocks_here * block_rows
    chosen = chosen_ref[:, 0, :]
    spread = (
        lax.broadcasted_iota(jnp.int32, (blocks_here, rows), 1) // block_rows
        == lax.broadcasted_iota(jnp.int32, (blocks_here, rows), 0)
    )
    spread = jnp.where(spread, 1.0, 0.0).astype(jnp.bfloat16)
    block_id = (
        my_index * blocks_here + lax.broadcasted_iota(jnp.int32, (1, rows), 1) // block_rows
    )
    named = named_pairs(chosen, block_id, block_id + 1, spread)
    key_at = lax.broadcasted_iota(jnp.int32, (rows, rows), 0)
    query_at = lax.broadcasted_iota(jnp.int32, (rows, rows), 1)
    allowed = named & (key_at <= query_at)
    far_rows = len(distances) * block_rows
    column = lax.broadcasted_iota(jnp.int32, (1, far_rows), 1)
    low = jnp.zeros((1, far_rows), jnp.int32)
    for at, distance in enumerate(distances):
        here = (column >= at * block_rows) & (column < (at + 1) * block_rows)
        low = jnp.where(here, jnp.bitwise_xor(my_index, distance) * blocks_here, low)
    far_named = named_pairs(chosen, low, low + blocks_here, spread)
    bias_ref[...] = jnp.where(far_named, 0.0, -jnp.inf)
    scale = HEAD_WIDTH ** (-0.5) * LOG2E
    for head in range(heads):
        lanes = slice(head * HEAD_WIDTH, (head + 1) * HEAD_WIDTH)
        raw = lax.dot_general(
            kv_ref[:, :HEAD_WIDTH],
            q_ref[:, lanes],
            (((1,), (1,)), ((), ())),
            preferred_element_type=jnp.float32,
        )
        raw = jnp.where(allowed, raw, -jnp.inf)
        top = jnp.max(raw, axis=0, keepdims=True)
        weights = jnp.exp2((raw - top) * scale)
        sum_ref[lanes, :] = lax.dot_general(
            kv_ref[:, HEAD_WIDTH:],
            weights.astype(jnp.bfloat16),
            (((0,), (0,)), ((), ())),
            preferred_element_type=jnp.float32,
        )
        stat_ref[head : head + 1, :] = top
        stat_ref[heads + head : heads + head + 1, :] = jnp.sum(weights, axis=0, keepdims=True)


def far_kernel(heads, far_count, bias_ref, q_ref, sum_ref, stat_ref, *refs):
    far_refs = refs[:far_count]
    out_ref, mass_ref = refs[far_count:]
    key_rows = jnp.concatenate([far[:, :HEAD_WIDTH] for far in far_refs], axis=0)
    value_rows = jnp.concatenate([far[:, HEAD_WIDTH:] for far in far_refs], axis=0)
    scale = HEAD_WIDTH ** (-0.5)
    for head in range(heads):
        lanes = slice(head * HEAD_WIDTH, (head + 1) * HEAD_WIDTH)
        raw = lax.dot_general(
            key_rows, q_ref[:, lanes], (((1,), (1,)), ((), ())), preferred_element_type=jnp.float32
        )
        raw = raw + bias_ref[...]
        near_top = stat_ref[head : head + 1, :]
        top = jnp.maximum(near_top, jnp.max(raw, axis=0, keepdims=True))
        weights = jnp.exp2((raw - top) * (scale * LOG2E))
        keep = jnp.exp2((near_top - top) * (scale * LOG2E))
        total = stat_ref[heads + head : heads + head + 1, :] * keep + jnp.sum(
            weights, axis=0, keepdims=True
        )
        summed = sum_ref[lanes, :] * keep + lax.dot_general(
            value_rows,
            weights.astype(jnp.bfloat16),
            (((0,), (0,)), ((), ())),
            preferred_element_type=jnp.float32,
        )
        out_ref[:, lanes] = (summed / total).T.astype(jnp.bfloat16)
        mass_ref[head : head + 1, :] = top * scale + jnp.log(total)


def mix_kernel(step, own_ref, other_ref, w_ref, out_ref):
    width = own_ref.shape[1]
    side = lax.axis_index("tp")
    lanes = pl.ds(pl.multiple_of(pl.program_id(0) * step, step), step)
    own_w = w_ref[pl.ds(pl.multiple_of(side * width, width), width), lanes]
    other_w = w_ref[pl.ds(pl.multiple_of((1 - side) * width, width), width), lanes]
    mixed = jnp.dot(own_ref[...], own_w, preferred_element_type=jnp.float32)
    mixed += jnp.dot(other_ref[...], other_w, preferred_element_type=jnp.float32)
    out_ref[...] = mixed.astype(jnp.bfloat16)


def body(tokens, w_query, key_weight, value_weight, w_out, chosen):
    local_tokens = tokens[0]
    local_chosen = jnp.transpose(chosen, (1, 0, 2))
    rows = local_tokens.shape[0]
    blocks_here = local_chosen.shape[0]
    block_rows = rows // blocks_here
    heads = w_query.shape[1] // HEAD_WIDTH
    count = lax.axis_size("kv")
    distances = xor_distances(count)
    far_count = len(distances)
    far_rows = far_count * block_rows
    asked = [exchange(local_chosen, distance, count) for distance in distances]

    def project(weight):
        return jnp.dot(local_tokens, weight, preferred_element_type=jnp.float32).astype(
            jnp.bfloat16
        )

    paired = jnp.concatenate([project(key_weight), project(value_weight)], axis=1)
    queries = project(w_query)
    width = queries.shape[1]
    block = jax.ShapeDtypeStruct((block_rows, paired.shape[1]), jnp.bfloat16)
    picked = pl.pallas_call(
        functools.partial(pick_kernel, blocks_here, block_rows, far_count),
        out_shape=[block] * far_count,
        in_specs=[VMEM] * (1 + far_count),
        out_specs=[VMEM] * far_count,
        compiler_params=grant(rows * width),
        name="pick",
    )(paired, *asked)
    far = [exchange(rows_out, distance, count) for rows_out, distance in zip(picked, distances)]
    near_sum, near_stat, far_bias = pl.pallas_call(
        functools.partial(local_kernel, blocks_here, block_rows, distances, heads),
        out_shape=[
            jax.ShapeDtypeStruct((width, rows), jnp.float32),
            jax.ShapeDtypeStruct((2 * heads, rows), jnp.float32),
            jax.ShapeDtypeStruct((far_rows, rows), jnp.float32),
        ],
        in_specs=[VMEM] * 3,
        out_specs=[VMEM] * 3,
        compiler_params=grant(rows * width, rows * rows, far_rows * rows),
        name="near",
    )(local_chosen, queries, paired)
    attended, log_mass = pl.pallas_call(
        functools.partial(far_kernel, heads, far_count),
        out_shape=[
            jax.ShapeDtypeStruct((rows, width), jnp.bfloat16),
            jax.ShapeDtypeStruct((heads, rows), jnp.float32),
        ],
        in_specs=[VMEM] * (4 + far_count),
        out_specs=[VMEM] * 2,
        compiler_params=grant(rows * width, 3 * far_rows * rows),
        name="far",
    )(far_bias, queries, near_sum, near_stat, *far)
    other = lax.ppermute(attended, "tp", [(0, 1), (1, 0)])
    columns = w_out.shape[1]
    step = columns // 4
    mixed = pl.pallas_call(
        functools.partial(mix_kernel, step),
        out_shape=jax.ShapeDtypeStruct((rows, columns), jnp.bfloat16),
        grid=(4,),
        in_specs=[VMEM] * 3,
        out_specs=pl.BlockSpec((rows, step), lambda at: (0, at)),
        compiler_params=grant(rows * columns),
        name="mix",
    )(attended, other, w_out)
    return (mixed[None], log_mass[None])


def solution(mesh):
    in_specs = (
        P("dp", "kv", None),
        P(None, "tp"),
        P(None, "tp"),
        P(None, "tp"),
        P(None, "tp"),
        P("dp", "kv", None),
    )
    out_specs = (P("dp", "kv", "tp"), P("dp", "tp", "kv"))
    return jax.shard_map(body, mesh=mesh, in_specs=in_specs, out_specs=out_specs, check_vma=False)
```

```python
import functools

import jax
import jax.numpy as jnp
from jax import lax
from jax.experimental import pallas as pl
from jax.experimental.pallas import tpu as pltpu
from jax.sharding import PartitionSpec as P


HEAD_WIDTH = 128
LOG2E = 1.4426950408889634
VMEM = pl.BlockSpec(memory_space=pltpu.VMEM)


def xor_distances(count):
    span = 1
    while span < count:
        span *= 2
    return list(range(1, span))


def exchange(value, distance, count):
    pairs = [(i, i ^ distance) for i in range(count) if (i ^ distance) < count]
    return lax.ppermute(value, "kv", pairs)


def shared_exchange(value, distances, count):
    pairs = [
        (2 * i + t, 2 * (i ^ distance) + t)
        for i in range(count)
        for t, distance in enumerate(distances)
        if (i ^ distance) < count
    ]
    return lax.ppermute(value, ("kv", "tp"), pairs)


def swap(value):
    return lax.ppermute(value, "tp", [(0, 1), (1, 0)])


def grant(*sizes):
    return pltpu.CompilerParams(vmem_limit_bytes=(4 << 20) + 4 * sum(sizes))


def project_kernel(
    chunks, tokens_ref, key_ref, value_ref, out_ref, tokens, weights, arrived
):
    width = key_ref.shape[1]
    step = key_ref.shape[0] // chunks
    copies = []
    for at in range(chunks):
        span = pl.ds(at * step, step)
        moves = (
            (tokens_ref.at[:, span], tokens.at[:, span]),
            (key_ref.at[span], weights.at[span, pl.ds(0, width)]),
            (value_ref.at[span], weights.at[span, pl.ds(width, width)]),
        )
        group = [
            pltpu.make_async_copy(source, target, arrived.at[at, lane])
            for lane, (source, target) in enumerate(moves)
        ]
        for copy in group:
            copy.start()
        copies.append(group)
    total = None
    for at in range(chunks):
        for copy in copies[at]:
            copy.wait()
        span = slice(at * step, (at + 1) * step)
        part = jnp.dot(tokens[:, span], weights[span, :], preferred_element_type=jnp.float32)
        total = part if total is None else total + part
    out_ref[...] = total.astype(jnp.bfloat16)


def pick_kernel(blocks_here, block_rows, shared_count, alone_count, kv_ref, kv_other_ref, *refs):
    asked_refs = refs[: shared_count + alone_count]
    out_refs = refs[shared_count + alone_count :]
    base = lax.axis_index("kv") * blocks_here
    rows = blocks_here * block_rows
    offset = lax.broadcasted_iota(jnp.int32, (block_rows, rows), 1) - lax.broadcasted_iota(
        jnp.int32, (block_rows, rows), 0
    )
    for at, (asked_ref, out_ref) in enumerate(zip(asked_refs, out_refs)):
        asked = asked_ref[:, 0, :]
        mine = (asked >= base) & (asked < base + blocks_here)
        local = jnp.max(jnp.where(mine, asked - base, -1), axis=(0, 1), keepdims=True)
        hot = jnp.where(offset == local * block_rows, 1.0, 0.0).astype(jnp.bfloat16)
        out_ref[:block_rows, :] = jnp.dot(
            hot, kv_ref[...], preferred_element_type=jnp.float32
        ).astype(jnp.bfloat16)
        if at < shared_count:
            out_ref[block_rows:, :] = jnp.dot(
                hot, kv_other_ref[...], preferred_element_type=jnp.float32
            ).astype(jnp.bfloat16)


def named_pairs(chosen, low, high, spread):
    member = (chosen[:, :1] >= low) & (chosen[:, :1] < high)
    for slot in range(1, chosen.shape[1]):
        entry = chosen[:, slot : slot + 1]
        member = member | ((entry >= low) & (entry < high))
    member = jnp.where(member, 1.0, 0.0).astype(jnp.bfloat16)
    return (
        lax.dot_general(
            member, spread, (((0,), (0,)), ((), ())), preferred_element_type=jnp.float32
        )
        > 0.5
    )


def local_kernel(
    blocks_here, block_rows, far_order, heads, chosen_ref, q_ref, kv_ref,
    sum_ref, stat_ref, bias_ref,
):
    my_index = lax.axis_index("kv")
    rows = blocks_here * block_rows
    chosen = chosen_ref[:, 0, :]
    spread = (
        lax.broadcasted_iota(jnp.int32, (blocks_here, rows), 1) // block_rows
        == lax.broadcasted_iota(jnp.int32, (blocks_here, rows), 0)
    )
    spread = jnp.where(spread, 1.0, 0.0).astype(jnp.bfloat16)
    block_id = (
        my_index * blocks_here + lax.broadcasted_iota(jnp.int32, (1, rows), 1) // block_rows
    )
    named = named_pairs(chosen, block_id, block_id + 1, spread)
    key_at = lax.broadcasted_iota(jnp.int32, (rows, rows), 0)
    query_at = lax.broadcasted_iota(jnp.int32, (rows, rows), 1)
    allowed = named & (key_at <= query_at)
    far_rows = len(far_order) * block_rows
    column = lax.broadcasted_iota(jnp.int32, (1, far_rows), 1)
    low = jnp.zeros((1, far_rows), jnp.int32)
    side = lax.axis_index("tp")
    for at, by_side in enumerate(far_order):
        here = (column >= at * block_rows) & (column < (at + 1) * block_rows)
        distance = jnp.where(side == 0, by_side[0], by_side[1])
        low = jnp.where(here, jnp.bitwise_xor(my_index, distance) * blocks_here, low)
    far_named = named_pairs(chosen, low, low + blocks_here, spread)
    bias_ref[...] = jnp.where(far_named, 0.0, -jnp.inf)
    scale = HEAD_WIDTH ** (-0.5) * LOG2E
    for head in range(heads):
        lanes = slice(head * HEAD_WIDTH, (head + 1) * HEAD_WIDTH)
        raw = lax.dot_general(
            kv_ref[:, :HEAD_WIDTH],
            q_ref[:, lanes],
            (((1,), (1,)), ((), ())),
            preferred_element_type=jnp.float32,
        )
        raw = jnp.where(allowed, raw, -jnp.inf)
        top = jnp.max(raw, axis=0, keepdims=True)
        weights = jnp.exp2((raw - top) * scale)
        sum_ref[lanes, :] = lax.dot_general(
            kv_ref[:, HEAD_WIDTH:],
            weights.astype(jnp.bfloat16),
            (((0,), (0,)), ((), ())),
            preferred_element_type=jnp.float32,
        )
        stat_ref[head : head + 1, :] = top
        stat_ref[heads + head : heads + head + 1, :] = jnp.sum(weights, axis=0, keepdims=True)


def far_kernel(
    heads, block_rows, shared_count, alone_count, bias_ref, q_ref, sum_ref, stat_ref, *refs
):
    out_ref, mass_ref = refs[-2:]
    far_refs = [ref.at[:block_rows] for ref in refs[: shared_count + alone_count]]
    far_refs += list(refs[shared_count + alone_count : -2])
    key_rows = jnp.concatenate([far[:, :HEAD_WIDTH] for far in far_refs], axis=0)
    value_rows = jnp.concatenate([far[:, HEAD_WIDTH:] for far in far_refs], axis=0)
    scale = HEAD_WIDTH ** (-0.5)
    for head in range(heads):
        lanes = slice(head * HEAD_WIDTH, (head + 1) * HEAD_WIDTH)
        raw = lax.dot_general(
            key_rows, q_ref[:, lanes], (((1,), (1,)), ((), ())), preferred_element_type=jnp.float32
        )
        raw = raw + bias_ref[...]
        near_top = stat_ref[head : head + 1, :]
        top = jnp.maximum(near_top, jnp.max(raw, axis=0, keepdims=True))
        weights = jnp.exp2((raw - top) * (scale * LOG2E))
        keep = jnp.exp2((near_top - top) * (scale * LOG2E))
        total = stat_ref[heads + head : heads + head + 1, :] * keep + jnp.sum(
            weights, axis=0, keepdims=True
        )
        summed = sum_ref[lanes, :] * keep + lax.dot_general(
            value_rows,
            weights.astype(jnp.bfloat16),
            (((0,), (0,)), ((), ())),
            preferred_element_type=jnp.float32,
        )
        out_ref[:, lanes] = (summed / total).T.astype(jnp.bfloat16)
        mass_ref[head : head + 1, :] = top * scale + jnp.log(total)


def half_mix_kernel(own_ref, w_ref, out_ref):
    width = own_ref.shape[1]
    start = lax.axis_index("tp") * width
    own_w = w_ref[pl.ds(pl.multiple_of(start, width), width), :]
    out_ref[...] = jnp.dot(own_ref[...], own_w, preferred_element_type=jnp.float32)


def mix_kernel(step, half_ref, other_ref, w_ref, out_ref):
    width = other_ref.shape[1]
    start = (1 - lax.axis_index("tp")) * width
    lanes = pl.ds(pl.multiple_of(pl.program_id(0) * step, step), step)
    other_w = w_ref[pl.ds(pl.multiple_of(start, width), width), lanes]
    mixed = half_ref[:, lanes] + jnp.dot(
        other_ref[...], other_w, preferred_element_type=jnp.float32
    )
    out_ref[...] = mixed.astype(jnp.bfloat16)


def body(tokens, w_query, key_weight, value_weight, w_out, chosen):
    local_tokens = tokens[0]
    local_chosen = jnp.transpose(chosen, (1, 0, 2))
    rows = local_tokens.shape[0]
    blocks_here = local_chosen.shape[0]
    block_rows = rows // blocks_here
    heads = w_query.shape[1] // HEAD_WIDTH
    count = lax.axis_size("kv")
    distances = xor_distances(count)
    shared = list(zip(distances[0:-1:2], distances[1::2]))
    alone = distances[2 * len(shared) :]
    shared_count, alone_count = len(shared), len(alone)
    far_order = shared + [(d, d) for d in alone] + [(b, a) for a, b in shared]
    far_rows = len(far_order) * block_rows
    asked = [shared_exchange(local_chosen, pair, count) for pair in shared]
    asked += [exchange(local_chosen, distance, count) for distance in alone]
    width = w_query.shape[1]
    pair_width = key_weight.shape[1] + value_weight.shape[1]
    depth = key_weight.shape[0]
    chunks = 4
    paired = pl.pallas_call(
        functools.partial(project_kernel, chunks),
        out_shape=jax.ShapeDtypeStruct((rows, pair_width), jnp.bfloat16),
        in_specs=[pl.BlockSpec(memory_space=pltpu.HBM)] * 3,
        out_specs=VMEM,
        scratch_shapes=[
            pltpu.VMEM((rows, depth), jnp.bfloat16),
            pltpu.VMEM((depth, pair_width), jnp.bfloat16),
            pltpu.SemaphoreType.DMA((chunks, 3)),
        ],
        compiler_params=grant(depth * pair_width, rows * depth),
        name="project",
    )(
        *[
            pltpu.with_memory_space_constraint(value, pltpu.HBM)
            for value in (local_tokens, key_weight, value_weight)
        ]
    )
    paired_other = swap(paired)
    queries = jnp.dot(local_tokens, w_query, preferred_element_type=jnp.float32).astype(
        jnp.bfloat16
    )
    two = jax.ShapeDtypeStruct((2 * block_rows, pair_width), jnp.bfloat16)
    one = jax.ShapeDtypeStruct((block_rows, pair_width), jnp.bfloat16)
    picked = pl.pallas_call(
        functools.partial(pick_kernel, blocks_here, block_rows, shared_count, alone_count),
        out_shape=[two] * shared_count + [one] * alone_count,
        in_specs=[VMEM] * (2 + shared_count + alone_count),
        out_specs=[VMEM] * (shared_count + alone_count),
        compiler_params=grant(rows * pair_width),
        name="pick",
    )(paired, paired_other, *asked)
    far = [shared_exchange(value, pair, count) for value, pair in zip(picked, shared)]
    far += [exchange(value, d, count) for value, d in zip(picked[shared_count:], alone)]
    if shared:
        crossing = [value[block_rows:] for value in far[:shared_count]]
        far.append(swap(jnp.concatenate(crossing, axis=0) if shared_count > 1 else crossing[0]))
    near_sum, near_stat, far_bias = pl.pallas_call(
        functools.partial(local_kernel, blocks_here, block_rows, far_order, heads),
        out_shape=[
            jax.ShapeDtypeStruct((width, rows), jnp.float32),
            jax.ShapeDtypeStruct((2 * heads, rows), jnp.float32),
            jax.ShapeDtypeStruct((far_rows, rows), jnp.float32),
        ],
        in_specs=[VMEM] * 3,
        out_specs=[VMEM] * 3,
        compiler_params=grant(rows * width, rows * rows, far_rows * rows),
        name="near",
    )(local_chosen, queries, paired)
    attended, log_mass = pl.pallas_call(
        functools.partial(far_kernel, heads, block_rows, shared_count, alone_count),
        out_shape=[
            jax.ShapeDtypeStruct((rows, width), jnp.bfloat16),
            jax.ShapeDtypeStruct((heads, rows), jnp.float32),
        ],
        in_specs=[VMEM] * (4 + len(far)),
        out_specs=[VMEM] * 2,
        compiler_params=grant(rows * width, 3 * far_rows * rows),
        name="far",
    )(far_bias, queries, near_sum, near_stat, *far)
    other = swap(attended)
    columns = w_out.shape[1]
    half = pl.pallas_call(
        half_mix_kernel,
        out_shape=jax.ShapeDtypeStruct((rows, columns), jnp.float32),
        in_specs=[VMEM] * 2,
        out_specs=VMEM,
        compiler_params=grant(rows * columns),
        name="half",
    )(attended, w_out)
    step = columns // 4
    mixed = pl.pallas_call(
        functools.partial(mix_kernel, step),
        out_shape=jax.ShapeDtypeStruct((rows, columns), jnp.bfloat16),
        grid=(4,),
        in_specs=[VMEM] * 3,
        out_specs=pl.BlockSpec((rows, step), lambda at: (0, at)),
        compiler_params=grant(rows * columns),
        name="mix",
    )(half, other, w_out)
    return (mixed[None], log_mass[None])


def solution(mesh):
    in_specs = (
        P("dp", "kv", None),
        P(None, "tp"),
        P(None, "tp"),
        P(None, "tp"),
        P(None, "tp"),
        P("dp", "kv", None),
    )
    out_specs = (P("dp", "kv", "tp"), P("dp", "tp", "kv"))
    return jax.shard_map(body, mesh=mesh, in_specs=in_specs, out_specs=out_specs, check_vma=False)
```

```python
import functools

import jax
import jax.numpy as jnp
from jax import lax
from jax.experimental import pallas as pl
from jax.experimental.pallas import tpu as pltpu
from jax.sharding import PartitionSpec as P


HEAD_WIDTH = 128
LOG2E = 1.4426950408889634
VMEM = pl.BlockSpec(memory_space=pltpu.VMEM)


def xor_distances(count):
    span = 1
    while span < count:
        span *= 2
    return [1, 3, *range(4, span), 2] if span > 2 else list(range(1, span))


def exchange(value, distance, count):
    pairs = [(i, i ^ distance) for i in range(count) if (i ^ distance) < count]
    return lax.ppermute(value, "kv", pairs)


def shared_exchange(value, distances, count):
    pairs = [
        (2 * i + t, 2 * (i ^ distance) + t)
        for i in range(count)
        for t, distance in enumerate(distances)
        if (i ^ distance) < count
    ]
    return lax.ppermute(value, ("kv", "tp"), pairs)


def swap(value):
    return lax.ppermute(value, "tp", [(0, 1), (1, 0)])


def grant(*sizes):
    return pltpu.CompilerParams(vmem_limit_bytes=(4 << 20) + 4 * sum(sizes))


def pick_kernel(blocks_here, block_rows, shared_count, alone_count, kv_ref, kv_other_ref, *refs):
    asked_refs = refs[: shared_count + alone_count]
    out_refs = refs[shared_count + alone_count :]
    base = lax.axis_index("kv") * blocks_here
    rows = blocks_here * block_rows
    offset = lax.broadcasted_iota(jnp.int32, (block_rows, rows), 1) - lax.broadcasted_iota(
        jnp.int32, (block_rows, rows), 0
    )
    for at, (asked_ref, out_ref) in enumerate(zip(asked_refs, out_refs)):
        asked = asked_ref[:, 0, :]
        mine = (asked >= base) & (asked < base + blocks_here)
        local = jnp.max(jnp.where(mine, asked - base, -1), axis=(0, 1), keepdims=True)
        hot = jnp.where(offset == local * block_rows, 1.0, 0.0).astype(jnp.bfloat16)
        out_ref[:block_rows, :] = jnp.dot(
            hot, kv_ref[...], preferred_element_type=jnp.float32
        ).astype(jnp.bfloat16)
        if at < shared_count:
            out_ref[block_rows:, :] = jnp.dot(
                hot, kv_other_ref[...], preferred_element_type=jnp.float32
            ).astype(jnp.bfloat16)


def named_pairs(chosen, low, high, spread):
    member = (chosen[:, :1] >= low) & (chosen[:, :1] < high)
    for slot in range(1, chosen.shape[1]):
        entry = chosen[:, slot : slot + 1]
        member = member | ((entry >= low) & (entry < high))
    member = jnp.where(member, 1.0, 0.0).astype(jnp.bfloat16)
    return (
        lax.dot_general(
            member, spread, (((0,), (0,)), ((), ())), preferred_element_type=jnp.float32
        )
        > 0.5
    )


def local_kernel(
    blocks_here, block_rows, far_order, heads, chosen_ref, q_ref, kv_ref,
    sum_ref, stat_ref, bias_ref,
):
    my_index = lax.axis_index("kv")
    rows = blocks_here * block_rows
    chosen = chosen_ref[:, 0, :]
    spread = (
        lax.broadcasted_iota(jnp.int32, (blocks_here, rows), 1) // block_rows
        == lax.broadcasted_iota(jnp.int32, (blocks_here, rows), 0)
    )
    spread = jnp.where(spread, 1.0, 0.0).astype(jnp.bfloat16)
    block_id = (
        my_index * blocks_here + lax.broadcasted_iota(jnp.int32, (1, rows), 1) // block_rows
    )
    named = named_pairs(chosen, block_id, block_id + 1, spread)
    key_at = lax.broadcasted_iota(jnp.int32, (rows, rows), 0)
    query_at = lax.broadcasted_iota(jnp.int32, (rows, rows), 1)
    allowed = named & (key_at <= query_at)
    far_rows = len(far_order) * block_rows
    column = lax.broadcasted_iota(jnp.int32, (1, far_rows), 1)
    low = jnp.zeros((1, far_rows), jnp.int32)
    side = lax.axis_index("tp")
    for at, by_side in enumerate(far_order):
        here = (column >= at * block_rows) & (column < (at + 1) * block_rows)
        distance = jnp.where(side == 0, by_side[0], by_side[1])
        low = jnp.where(here, jnp.bitwise_xor(my_index, distance) * blocks_here, low)
    far_named = named_pairs(chosen, low, low + blocks_here, spread)
    bias_ref[...] = jnp.where(far_named, 0.0, -jnp.inf)
    scale = HEAD_WIDTH ** (-0.5) * LOG2E
    for head in range(heads):
        lanes = slice(head * HEAD_WIDTH, (head + 1) * HEAD_WIDTH)
        raw = lax.dot_general(
            kv_ref[:, :HEAD_WIDTH],
            q_ref[:, lanes],
            (((1,), (1,)), ((), ())),
            preferred_element_type=jnp.float32,
        )
        raw = jnp.where(allowed, raw, -jnp.inf)
        top = jnp.max(raw, axis=0, keepdims=True)
        weights = jnp.exp2((raw - top) * scale)
        sum_ref[lanes, :] = lax.dot_general(
            kv_ref[:, HEAD_WIDTH:],
            weights.astype(jnp.bfloat16),
            (((0,), (0,)), ((), ())),
            preferred_element_type=jnp.float32,
        )
        stat_ref[head : head + 1, :] = top
        stat_ref[heads + head : heads + head + 1, :] = jnp.sum(weights, axis=0, keepdims=True)


def far_kernel(
    heads, block_rows, shared_count, alone_count, bias_ref, q_ref, sum_ref, stat_ref, *refs
):
    out_ref, mass_ref = refs[-2:]
    far_refs = [ref.at[:block_rows] for ref in refs[: shared_count + alone_count]]
    far_refs += list(refs[shared_count + alone_count : -2])
    key_rows = jnp.concatenate([far[:, :HEAD_WIDTH] for far in far_refs], axis=0)
    value_rows = jnp.concatenate([far[:, HEAD_WIDTH:] for far in far_refs], axis=0)
    scale = HEAD_WIDTH ** (-0.5)
    for head in range(heads):
        lanes = slice(head * HEAD_WIDTH, (head + 1) * HEAD_WIDTH)
        raw = lax.dot_general(
            key_rows, q_ref[:, lanes], (((1,), (1,)), ((), ())), preferred_element_type=jnp.float32
        )
        raw = raw + bias_ref[...]
        near_top = stat_ref[head : head + 1, :]
        top = jnp.maximum(near_top, jnp.max(raw, axis=0, keepdims=True))
        weights = jnp.exp2((raw - top) * (scale * LOG2E))
        keep = jnp.exp2((near_top - top) * (scale * LOG2E))
        total = stat_ref[heads + head : heads + head + 1, :] * keep + jnp.sum(
            weights, axis=0, keepdims=True
        )
        summed = sum_ref[lanes, :] * keep + lax.dot_general(
            value_rows,
            weights.astype(jnp.bfloat16),
            (((0,), (0,)), ((), ())),
            preferred_element_type=jnp.float32,
        )
        out_ref[:, lanes] = (summed / total).T.astype(jnp.bfloat16)
        mass_ref[head : head + 1, :] = top * scale + jnp.log(total)


def half_mix_kernel(own_ref, w_ref, out_ref):
    width = own_ref.shape[1]
    start = lax.axis_index("tp") * width
    own_w = w_ref[pl.ds(pl.multiple_of(start, width), width), :]
    out_ref[...] = jnp.dot(own_ref[...], own_w, preferred_element_type=jnp.float32)


def mix_kernel(chunks, half_ref, other_ref, w_ref, out_ref, mixed_ref, sent):
    rows, width = other_ref.shape
    start = (1 - lax.axis_index("tp")) * width
    other_w = w_ref[pl.ds(pl.multiple_of(start, width), width), :]
    step = rows // chunks
    copies = []
    for at in range(chunks):
        span = slice(at * step, (at + 1) * step)
        mixed = half_ref[span, :] + jnp.dot(
            other_ref[span, :], other_w, preferred_element_type=jnp.float32
        )
        mixed_ref[span, :] = mixed.astype(jnp.bfloat16)
        copy = pltpu.make_async_copy(mixed_ref.at[span], out_ref.at[span], sent.at[at])
        copy.start()
        copies.append(copy)
    for copy in copies:
        copy.wait()


def body(tokens, w_query, key_weight, value_weight, w_out, chosen):
    local_tokens = tokens[0]
    local_chosen = jnp.transpose(chosen, (1, 0, 2))
    rows = local_tokens.shape[0]
    blocks_here = local_chosen.shape[0]
    block_rows = rows // blocks_here
    heads = w_query.shape[1] // HEAD_WIDTH
    count = lax.axis_size("kv")
    distances = xor_distances(count)
    shared = list(zip(distances[0:-1:2], distances[1::2]))
    alone = distances[2 * len(shared) :]
    shared_count, alone_count = len(shared), len(alone)
    far_order = shared + [(d, d) for d in alone] + [(b, a) for a, b in shared]
    far_rows = len(far_order) * block_rows
    asked = [shared_exchange(local_chosen, pair, count) for pair in shared]
    asked += [exchange(local_chosen, distance, count) for distance in alone]
    width = w_query.shape[1]
    pair_width = key_weight.shape[1] + value_weight.shape[1]

    def project(weight):
        return jnp.dot(local_tokens, weight, preferred_element_type=jnp.float32).astype(
            jnp.bfloat16
        )

    paired = jnp.concatenate([project(key_weight), project(value_weight)], axis=1)
    paired_other = swap(paired)
    queries = project(w_query)
    two = jax.ShapeDtypeStruct((2 * block_rows, pair_width), jnp.bfloat16)
    one = jax.ShapeDtypeStruct((block_rows, pair_width), jnp.bfloat16)
    picked = pl.pallas_call(
        functools.partial(pick_kernel, blocks_here, block_rows, shared_count, alone_count),
        out_shape=[two] * shared_count + [one] * alone_count,
        in_specs=[VMEM] * (2 + shared_count + alone_count),
        out_specs=[VMEM] * (shared_count + alone_count),
        compiler_params=grant(rows * pair_width),
        name="pick",
    )(paired, paired_other, *asked)
    far = [shared_exchange(value, pair, count) for value, pair in zip(picked, shared)]
    far += [exchange(value, d, count) for value, d in zip(picked[shared_count:], alone)]
    if shared:
        crossing = [value[block_rows:] for value in far[:shared_count]]
        far.append(swap(jnp.concatenate(crossing, axis=0) if shared_count > 1 else crossing[0]))
    near_sum, near_stat, far_bias = pl.pallas_call(
        functools.partial(local_kernel, blocks_here, block_rows, far_order, heads),
        out_shape=[
            jax.ShapeDtypeStruct((width, rows), jnp.float32),
            jax.ShapeDtypeStruct((2 * heads, rows), jnp.float32),
            jax.ShapeDtypeStruct((far_rows, rows), jnp.float32),
        ],
        in_specs=[VMEM] * 3,
        out_specs=[VMEM] * 3,
        compiler_params=grant(rows * width, rows * rows, far_rows * rows),
        name="near",
    )(local_chosen, queries, paired)
    attended, log_mass = pl.pallas_call(
        functools.partial(far_kernel, heads, block_rows, shared_count, alone_count),
        out_shape=[
            jax.ShapeDtypeStruct((rows, width), jnp.bfloat16),
            jax.ShapeDtypeStruct((heads, rows), jnp.float32),
        ],
        in_specs=[VMEM] * (4 + len(far)),
        out_specs=[VMEM] * 2,
        compiler_params=grant(rows * width, 3 * far_rows * rows),
        name="far",
    )(far_bias, queries, near_sum, near_stat, *far)
    other = swap(attended)
    columns = w_out.shape[1]
    half = pl.pallas_call(
        half_mix_kernel,
        out_shape=jax.ShapeDtypeStruct((rows, columns), jnp.float32),
        in_specs=[VMEM] * 2,
        out_specs=VMEM,
        compiler_params=grant(rows * columns),
        name="half",
    )(attended, w_out)
    mix_chunks = 2
    mixed = pl.pallas_call(
        functools.partial(mix_kernel, mix_chunks),
        out_shape=jax.ShapeDtypeStruct((rows, columns), jnp.bfloat16),
        in_specs=[VMEM] * 3,
        out_specs=pl.BlockSpec(memory_space=pltpu.HBM),
        scratch_shapes=[
            pltpu.VMEM((rows, columns), jnp.bfloat16),
            pltpu.SemaphoreType.DMA((mix_chunks,)),
        ],
        compiler_params=grant(rows * columns),
        name="mix",
    )(half, other, w_out)
    return (mixed[None], log_mass[None])


def solution(mesh):
    in_specs = (
        P("dp", "kv", None),
        P(None, "tp"),
        P(None, "tp"),
        P(None, "tp"),
        P(None, "tp"),
        P("dp", "kv", None),
    )
    out_specs = (P("dp", "kv", "tp"), P("dp", "tp", "kv"))
    return jax.shard_map(body, mesh=mesh, in_specs=in_specs, out_specs=out_specs, check_vma=False)
```
